32 devices in a mesh: sp: 4 (over z), fs: 4 (over y, x), tp: 2 (over core).
Axes of the slice: x: 2, y: 2, z: 4, core: 2. Of those that a mesh axis runs over, the one named last changes fastest.
Arguments:
- tokens: bfloat16 [8, 1536, 2048], P('fs', ('sp', 'tp')), may hold values from -6 to 6
- norm_gain: float32 [2048], replicated, may hold values from 0.1 to 1.9
- chain_entry: bfloat16 [2048, 2048], P(('sp', 'fs'), 'tp'), may hold values from -0.125 to 0.125
- pool_entry: bfloat16 [2048, 2048], P(('sp', 'fs'), 'tp'), may hold values from -0.125 to 0.125
- conv_taps: bfloat16 [4, 2048], P(None, 'tp'), may hold values from -3 to 3
- recur_gate: bfloat16 [8, 256, 256], P('tp'), may hold values from -0.375 to 0.375
- input_gate: bfloat16 [8, 256, 256], P('tp'), may hold values from -0.375 to 0.375
- decay_log: float32 [2048], P('tp'), may hold values from -9 to 5
- decay_shift: float32 [8, 1536, 2048], P('fs', 'sp', 'tp'), may hold values from -1 to 0
- start_state: float32 [8, 2048], P('fs', 'tp'), may hold values from -6 to 6
- pool_mix: bfloat16 [8, 256, 256], P('tp'), may hold values from -0.375 to 0.375
- pool_scale: float32 [2048], P('tp'), may hold values from 0.1 to 1.9
- chain_exit: bfloat16 [2048, 2048], P('tp', ('sp', 'fs')), may hold values from -0.09375 to 0.09375
- pool_exit: bfloat16 [2048, 2048], P('tp', ('sp', 'fs')), may hold values from -0.09375 to 0.09375
Outputs:
- mixed_rows: bfloat16 [8, 1536, 2048], P('fs', ('sp', 'tp'))
The draws below stay inside these ranges and needn't reach their ends.
All inputs are finite; a program needn't handle non-finite values.
Results may differ from the reference program's by a relative error of at most 0.01.
Values may be sent and summed in bfloat16 or wider, within the bound.
No kernel may reach another device: no remote copies, remote signals or barrier semaphores. Data moves between devices by JAX's collectives and lax.ppermute only.
A program may use at most 128 MiB of HBM per device.

```python
import math
import jax
import jax.numpy as jnp
from jax import lax

D = 2048
HEAD = 256
CHAIN_HEADS = 8
POOL_GROUPS = 8
CONV_TAPS = 4
POOL_SPAN = 16
TOK_DEV = 384
CHAIN_WIDTH = 2048
POOL_WIDTH = 2048
LEN = 1536
SEQS = 8


def draw_decay_log(key, part):
    inner = jax.random.fold_in(key, 7)
    return jax.random.uniform(inner, (CHAIN_WIDTH,), jnp.float32, -9.0, 5.0)


def draw_decay_shift(key, part):
    inner = jax.random.fold_in(key, 11)
    first_key, second_key, third_key, fourth_key, fifth_key, sixth_key, seventh_key = jax.random.split(inner, 7)
    block_span = TOK_DEV // 4
    block_total = SEQS * LEN // block_span
    slowness = jnp.exp(jax.random.uniform(first_key, (block_total, 1, CHAIN_WIDTH), jnp.float32, math.log(0.1), math.log(0.8)))
    jitter = jax.random.uniform(second_key, (block_total, block_span, CHAIN_WIDTH), jnp.float32, 0.5, 1.5)
    fast_share = 0.5
    fast_pick = jax.random.uniform(fifth_key, (CHAIN_WIDTH,), jnp.float32) < fast_share
    fast_rate = jnp.exp(jax.random.uniform(sixth_key, (CHAIN_WIDTH,), jnp.float32, math.log(0.012), math.log(0.035)))
    fast_boost = jnp.exp(jax.random.uniform(seventh_key, (block_total, 1, CHAIN_WIDTH), jnp.float32, math.log(0.6), math.log(1.6)))
    rate = slowness / LEN + jnp.where(fast_pick, fast_rate, 0.0)[None, None, :] * fast_boost
    steady = -(rate * jitter).reshape(SEQS, LEN, CHAIN_WIDTH)
    places = jax.random.randint(third_key, (SEQS, 4), 0, LEN)
    struck = jnp.any(jnp.arange(LEN)[None, :, None] == places[:, None, :], axis=2)
    depth = jax.random.uniform(fourth_key, (SEQS, LEN, CHAIN_WIDTH), jnp.float32, -0.7, -0.2)
    return steady + jnp.where(struck[:, :, None], depth, 0.0)


def steps_of(stream_key, extent, pieces, least, high):
    level, own = 1.0, jax.random.fold_in(stream_key, 6)
    for dim, shards_of in pieces:
        heights = jnp.exp(jax.random.uniform(jax.random.fold_in(own, dim), (shards_of,), jnp.float32, least / len(pieces), high / len(pieces)))
        level = level * jnp.repeat(heights, extent[dim] // shards_of).reshape([-1 if axis == dim else 1 for axis in range(len(extent))])
    return level


def scatter_about(stream_key, dims, width, reach, pieces=(), kind=jnp.bfloat16):
    array = width * jax.random.normal(stream_key, dims, jnp.float32)
    if pieces:
        array = array * steps_of(stream_key, dims, pieces, -0.22, 0.18)
    return jnp.clip(array, -reach, reach).astype(kind)


def setup_inputs(seed: int = 0) -> dict:
    seeds = jax.random.split(jax.random.key(seed), 15)
    return {
        "tokens": scatter_about(seeds[0], (SEQS, LEN, D), 1.0, 6.0, ((0, 4), (1, 8))),
        "norm_gain": jnp.clip(1.0 + 0.18 * jax.random.normal(seeds[1], (D,), jnp.float32), 0.1, 1.9),
        "chain_entry": scatter_about(seeds[2], (D, CHAIN_WIDTH), D ** -0.5, 0.125, ((0, 16), (1, 2))),
        "pool_entry": scatter_about(seeds[3], (D, POOL_WIDTH), D ** -0.5, 0.125, ((0, 16), (1, 2))),
        "conv_taps": scatter_about(seeds[4], (CONV_TAPS, CHAIN_WIDTH), CONV_TAPS ** -0.5, 3.0, ((1, 2),)),
        "recur_gate": scatter_about(seeds[5], (CHAIN_HEADS, HEAD, HEAD), HEAD ** -0.5, 0.375, ((0, 2),)),
        "input_gate": scatter_about(seeds[6], (CHAIN_HEADS, HEAD, HEAD), HEAD ** -0.5, 0.375, ((0, 2),)),
        "decay_log": draw_decay_log(jax.random.fold_in(seeds[14], 71), 0),
        "decay_shift": draw_decay_shift(jax.random.fold_in(seeds[14], 71), 0),
        "start_state": scatter_about(seeds[9], (SEQS, CHAIN_WIDTH), 1.0, 6.0, ((0, 4), (1, 2)), jnp.float32),
        "pool_mix": scatter_about(seeds[10], (POOL_GROUPS, HEAD, HEAD), HEAD ** -0.5, 0.375, ((0, 2),)),
        "pool_scale": jnp.clip(1.0 + 0.18 * jax.random.normal(seeds[11], (POOL_WIDTH,), jnp.float32), 0.1, 1.9),
        "chain_exit": scatter_about(seeds[12], (CHAIN_WIDTH, D), (CHAIN_WIDTH + POOL_WIDTH) ** -0.5, 0.09375, ((0, 2), (1, 16))),
        "pool_exit": scatter_about(seeds[13], (POOL_WIDTH, D), (CHAIN_WIDTH + POOL_WIDTH) ** -0.5, 0.09375, ((0, 2), (1, 16))),
    }


NORM_EPSILON = 1e-06
RECUR_SCALE = 8.0

def block_map(values, weight):
    row_total = values.shape[0]
    groups, block_width, _ = weight.shape
    blocks = values.astype(jnp.float32).reshape(row_total, groups, block_width)
    mapped = jnp.einsum('sgi,gij->sgj', blocks, weight.astype(jnp.float32))
    return mapped.reshape(row_total, groups * block_width)

def combine(earlier, latter):
    return (earlier[0] * latter[0], latter[0] * earlier[1] + latter[1])

def trailing(padded, row_total, window_id):
    sum_two = padded[1:] + padded[:-1]
    sum_four = sum_two[2:] + sum_two[:-2]
    sum_eight = sum_four[4:] + sum_four[:-4]
    sixteen = sum_eight[8:] + sum_eight[:-8]
    return jnp.where(window_id == 0, sum_two[-row_total:], jnp.where(window_id == 1, sum_four[-row_total:], jnp.where(window_id == 2, sum_eight[-row_total:], sixteen[-row_total:])))

def reference(tokens, norm_gain, chain_entry, pool_entry, conv_taps, recur_gate, input_gate, decay_log, decay_shift, start_state, pool_mix, pool_scale, chain_exit, pool_exit):
    channel = jnp.arange(POOL_WIDTH, dtype=jnp.int32) // HEAD
    window_id = (channel % 4)[None, :]
    window = jnp.power(2.0, (window_id + 1).astype(jnp.float32))
    position = jnp.arange(LEN, dtype=jnp.float32)[:, None]
    counts = jnp.minimum(position + 1.0, window)
    decay_rate = jnp.exp(decay_log) / LEN

    def one_sequence(inputs):
        values, shift_rows, begin_state = inputs
        widened = values.astype(jnp.float32)
        normed = (widened * lax.rsqrt(lax.optimization_barrier(jnp.mean(widened * widened, axis=-1, keepdims=True)) + NORM_EPSILON) * norm_gain.astype(jnp.float32)).astype(jnp.bfloat16)
        chain_input = jnp.dot(normed, chain_entry, preferred_element_type=jnp.float32).astype(jnp.bfloat16)
        pool_input = jnp.dot(normed, pool_entry, preferred_element_type=jnp.float32).astype(jnp.bfloat16)
        padded = jnp.pad(chain_input.astype(jnp.float32), ((CONV_TAPS - 1, 0), (0, 0)))
        conv_out = jnp.zeros((LEN, CHAIN_WIDTH), jnp.float32)
        for offset in range(CONV_TAPS):
            conv_out = conv_out + padded[offset:offset + LEN] * conv_taps[offset].astype(jnp.float32)
        conv_out = conv_out.astype(jnp.bfloat16)
        gate_recur = jax.nn.sigmoid(block_map(conv_out, recur_gate))
        gate_input = jax.nn.sigmoid(block_map(conv_out, input_gate))
        log_decay = -RECUR_SCALE * gate_recur * decay_rate + shift_rows
        decay_factor = jnp.exp(log_decay)
        drive_term = jnp.sqrt(-jnp.expm1(2.0 * log_decay)) * gate_input * conv_out.astype(jnp.float32)
        drive_term = drive_term.at[0].add(decay_factor[0] * begin_state)
        state = lax.associative_scan(combine, (decay_factor, drive_term), axis=0)[1]
        recurrent = state.astype(jnp.bfloat16)
        pool_pad = jnp.pad(pool_input.astype(jnp.float32), ((POOL_SPAN - 1, 0), (0, 0)))
        trail_sum = trailing(pool_pad, LEN, window_id)
        pool_diff = (trail_sum / counts - pool_input.astype(jnp.float32)).astype(jnp.bfloat16)
        pooled = (block_map(pool_diff, pool_mix) * pool_scale.astype(jnp.float32)).astype(jnp.bfloat16)
        mixed_rows = jnp.dot(recurrent, chain_exit, preferred_element_type=jnp.float32) + jnp.dot(pooled, pool_exit, preferred_element_type=jnp.float32)
        return mixed_rows.astype(jnp.bfloat16)
    return lax.map(one_sequence, (tokens, decay_shift, start_state))
```

```python
import functools
import math

import jax
import jax.numpy as jnp
from jax import lax
from jax.experimental import pallas as pl
from jax.experimental.pallas import tpu as pltpu
from jax.sharding import PartitionSpec as P


HALO = 16
LANES = 128
NORM_EPSILON = 1e-06
RECUR_SCALE = 8.0
CHUNKS = 8
VMEM_LIMIT = 60 * 1024 * 1024
ROUTES = {"ce": "zxy", "pe": "zyx", "cx": "xzy", "px": "yzx"}


def ring_pairs(size):
    return [(i, (i + 1) % size) for i in range(size)]


def swap_pairs(size, bit):
    return [(i, i ^ bit) for i in range(size)]


def gather_blocks(own, route, sp_n, fs_n):
    parts = [(own[None], [(0, 0)])]
    for step in route:
        if step == "z":
            held = jnp.concatenate([p[0] for p in parts], axis=0) if len(parts) > 1 else parts[0][0]
            places = [q for p in parts for q in p[1]]
            parts = [(held, places)]
            for lap in range(1, sp_n):
                held = lax.ppermute(held, "sp", ring_pairs(sp_n))
                parts.append((held, [(f, lap) for f, _ in places]))
            if route.index(step) < 2:
                parts = [
                    (
                        jnp.concatenate([p[0] for p in parts], axis=0),
                        [q for p in parts for q in p[1]],
                    )
                ]
        else:
            bit = 1 if step == "x" else 2
            parts = parts + [
                (
                    lax.ppermute(stack, "fs", swap_pairs(fs_n, bit)),
                    [(f ^ bit, s) for f, s in places],
                )
                for stack, places in parts
            ]
    return [(stack, [f * sp_n + s for f, s in places]) for stack, places in parts]


def norm_kernel(order, side, own, other, halo, gain, out):
    blocks = own.shape[2] // LANES
    half = own.shape[1]

    def rows_of(src, start, base, count, size):
        def one(i, _):
            at = pl.multiple_of(start + i * size, size)
            wide = src[0, pl.ds(at, size), :].astype(jnp.float32)
            scale = lax.rsqrt(jnp.mean(wide * wide, axis=-1, keepdims=True) + NORM_EPSILON)
            to = pl.multiple_of(base + i * size, size)
            for b in range(blocks):
                col = pl.multiple_of(order[b] * LANES, LANES)
                part = src[0, pl.ds(at, size), pl.ds(col, LANES)].astype(jnp.float32)
                out[0, pl.ds(to, size), b * LANES : (b + 1) * LANES] = (
                    part * scale * gain[:, pl.ds(col, LANES)]
                ).astype(out.dtype)
            return 0

        lax.fori_loop(0, count, one, 0)

    rows_of(halo, 0, 0, 1, HALO)
    rows_of(own, 0, HALO + side[0] * half, half // HALO, HALO)
    rows_of(other, 0, HALO + (1 - side[0]) * half, half // HALO, HALO)


def norm_rows(order, side, own, other, halo, gain):
    seqs, half, width = own.shape
    rows = 2 * half + HALO
    return pl.pallas_call(
        norm_kernel,
        out_shape=jax.ShapeDtypeStruct((seqs, rows, width), jnp.bfloat16),
        grid_spec=pltpu.PrefetchScalarGridSpec(
            num_scalar_prefetch=2,
            grid=(seqs,),
            in_specs=[
                pl.BlockSpec((1, half, width), lambda i, *_: (i, 0, 0)),
                pl.BlockSpec((1, half, width), lambda i, *_: (i, 0, 0)),
                pl.BlockSpec((1, HALO, width), lambda i, *_: (i, 0, 0)),
                pl.BlockSpec((1, width), lambda i, *_: (0, 0)),
            ],
            out_specs=pl.BlockSpec((1, rows, width), lambda i, *_: (i, 0, 0)),
        ),
        compiler_params=pltpu.CompilerParams(vmem_limit_bytes=VMEM_LIMIT),
        cost_estimate=pl.CostEstimate(flops=4_000_000_000, transcendentals=0, bytes_accessed=8_000_000),
        name="norm_rows",
    )(order, side, own, other, halo, gain.reshape(1, width))


def entry_kernel(places, tile, x, *refs):
    stacks, (out, held, sems) = refs[: len(places)], refs[len(places) :]
    depth = stacks[0].shape[1]
    width = out.shape[1]
    tiles = width // tile

    def copies(j):
        col = j * tile
        return [
            pltpu.make_async_copy(
                stack.at[m, :, pl.ds(col, tile)],
                held.at[j, pl.ds(r * depth, depth), :],
                sems.at[j, r],
            )
            for stack, places_of in zip(stacks, places)
            for m, r in enumerate(places_of)
        ]

    for j in range(tiles):
        for copy in copies(j):
            copy.start()
    for j in range(tiles):
        for copy in copies(j):
            copy.wait()
        out[:, j * tile : (j + 1) * tile] = jnp.dot(
            x[...], held[j], preferred_element_type=jnp.float32
        ).astype(out.dtype)


def entry_dot(x, parts, name):
    rows, depth = x.shape
    width = parts[0][0].shape[2]
    tile = min(256, width)
    places = [p[1] for p in parts]
    shards = sum(len(p) for p in places)
    return pl.pallas_call(
        functools.partial(entry_kernel, places, tile),
        out_shape=jax.ShapeDtypeStruct((rows, width), jnp.bfloat16),
        in_specs=[pl.BlockSpec(memory_space=pltpu.VMEM)]
        + [pl.BlockSpec(memory_space=pl.ANY)] * len(parts),
        out_specs=pl.BlockSpec(memory_space=pltpu.VMEM),
        scratch_shapes=[
            pltpu.VMEM((width // tile, depth, tile), jnp.bfloat16),
            pltpu.SemaphoreType.DMA((width // tile, shards)),
        ],
        compiler_params=pltpu.CompilerParams(vmem_limit_bytes=VMEM_LIMIT),
        cost_estimate=pl.CostEstimate(
            flops=2 * rows * depth * width, transcendentals=0, bytes_accessed=2 * depth * width
        ),
        name=name,
    )(x, *[p[0] for p in parts])


def chain_kernel(length, x, taps, wr, wi, rate_log, shift, h_out, p_out, seam_h, seam_p, wide, a_at, u_at):
    rows = shift.shape[1]
    span = rows // CHUNKS
    tap_count = taps.shape[0]
    wide[...] = x[0].astype(jnp.float32)
    first = HALO - (tap_count - 1)
    conv = wide[first : first + rows, :] * taps[0:1, :].astype(jnp.float32)
    for j in range(1, tap_count):
        conv = conv + wide[first + j : first + j + rows, :] * taps[j : j + 1, :].astype(jnp.float32)
    conv = conv.astype(jnp.bfloat16)
    to_recur = jnp.dot(conv, wr[0], preferred_element_type=jnp.float32)
    to_input = jnp.dot(conv, wi[0], preferred_element_type=jnp.float32)
    gate_recur = 0.5 * jnp.tanh(0.5 * to_recur) + 0.5
    gate_input = 0.5 * jnp.tanh(0.5 * to_input) + 0.5
    rate = jnp.exp(rate_log[...]) * (-RECUR_SCALE / length)
    log_decay = gate_recur * rate + shift[0]
    decay = jnp.exp(log_decay)
    twice = 2.0 * log_decay
    series = 1.0 + twice * (1.0 / 8.0)
    for k in range(7, 1, -1):
        series = 1.0 + twice * (1.0 / k) * series
    gone = jnp.where(twice > -0.5, -twice * series, 1.0 - decay * decay)
    root = gone * lax.rsqrt(jnp.maximum(gone, 1e-37))
    drive = root * gate_input * conv.astype(jnp.float32)
    width = wide.shape[1]
    lanes = [slice(b * LANES, (b + 1) * LANES) for b in range(width // LANES)]
    for b, cols in enumerate(lanes):
        a_at[b] = decay[:, cols]
        u_at[b] = drive[:, cols]
    states = [jnp.zeros((CHUNKS, LANES), jnp.float32) for _ in lanes]
    keeps = [jnp.ones((CHUNKS, LANES), jnp.float32) for _ in lanes]
    for t in range(span):
        step = pl.ds(t, CHUNKS, stride=span)
        for b in range(len(lanes)):
            a = a_at[b, step, :]
            states[b] = a * states[b] + u_at[b, step, :]
            keeps[b] = a * keeps[b]
            u_at[b, step, :] = states[b]
            a_at[b, step, :] = keeps[b]
    state = jnp.concatenate(states, axis=1)
    kept = jnp.concatenate(keeps, axis=1)
    for b, cols in enumerate(lanes):
        h_out[0, :, cols] = u_at[b]
        p_out[0, :, cols] = a_at[b]
    before_h = jnp.zeros((1, width), jnp.float32)
    before_p = jnp.ones((1, width), jnp.float32)
    for c in range(CHUNKS):
        seam_h[0, c : c + 1, :] = before_h
        seam_p[0, c : c + 1, :] = before_p
        before_h = kept[c : c + 1] * before_h + state[c : c + 1]
        before_p = kept[c : c + 1] * before_p
    seam_h[0, CHUNKS : 2 * CHUNKS, :] = jnp.broadcast_to(before_h, (CHUNKS, width))
    seam_p[0, CHUNKS : 2 * CHUNKS, :] = jnp.broadcast_to(before_p, (CHUNKS, width))


def chain_scan(x, taps, wr, wi, rate_log, shift, length):
    seqs, rows, width = shift.shape
    heads, head, _ = wr.shape
    return pl.pallas_call(
        functools.partial(chain_kernel, length),
        out_shape=(
            jax.ShapeDtypeStruct((seqs, rows, width), jnp.float32),
            jax.ShapeDtypeStruct((seqs, rows, width), jnp.float32),
            jax.ShapeDtypeStruct((seqs, 2 * CHUNKS, width), jnp.float32),
            jax.ShapeDtypeStruct((seqs, 2 * CHUNKS, width), jnp.float32),
        ),
        grid=(seqs, heads),
        in_specs=[
            pl.BlockSpec((1, rows + HALO, head), lambda i, g: (i, 0, g)),
            pl.BlockSpec((taps.shape[0], head), lambda i, g: (0, g)),
            pl.BlockSpec((1, head, head), lambda i, g: (g, 0, 0)),
            pl.BlockSpec((1, head, head), lambda i, g: (g, 0, 0)),
            pl.BlockSpec((1, head), lambda i, g: (0, g)),
            pl.BlockSpec((1, rows, head), lambda i, g: (i, 0, g)),
        ],
        out_specs=(
            pl.BlockSpec((1, rows, head), lambda i, g: (i, 0, g)),
            pl.BlockSpec((1, rows, head), lambda i, g: (i, 0, g)),
            pl.BlockSpec((1, 2 * CHUNKS, head), lambda i, g: (i, 0, g)),
            pl.BlockSpec((1, 2 * CHUNKS, head), lambda i, g: (i, 0, g)),
        ),
        scratch_shapes=[
            pltpu.VMEM((rows + HALO, head), jnp.float32),
            pltpu.VMEM((head // LANES, rows, LANES), jnp.float32),
            pltpu.VMEM((head // LANES, rows, LANES), jnp.float32),
        ],
        compiler_params=pltpu.CompilerParams(vmem_limit_bytes=VMEM_LIMIT),
        cost_estimate=pl.CostEstimate(
            flops=8_000_000_000, transcendentals=0, bytes_accessed=12_000_000
        ),
        name="chain_scan",
    )(x, taps, wr, wi, rate_log.reshape(1, width), shift)


def pool_kernel(start, x, mix, scale, out, wide, two, four, eight):
    rows = out.shape[1]
    total = rows + HALO
    group = lax.rem(pl.program_id(1), 4)
    for ref in (wide, two, four, eight):
        ref[0:8, :] = jnp.zeros((8, ref.shape[1]), jnp.float32)
    low, high = 8, 8 + total
    wide[low:high, :] = x[0].astype(jnp.float32)
    two[low:high, :] = wide[low:high, :] + wide[low - 1 : high - 1, :]
    four[low:high, :] = two[low:high, :] + two[low - 2 : high - 2, :]
    eight[low:high, :] = four[low:high, :] + four[low - 4 : high - 4, :]
    first = low + HALO
    sum_two = two[first:high, :]
    sum_four = four[first:high, :]
    sum_eight = eight[first:high, :]
    sixteen = sum_eight + eight[first - 8 : high - 8, :]
    trail = jnp.where(
        group == 0, sum_two, jnp.where(group == 1, sum_four, jnp.where(group == 2, sum_eight, sixteen))
    )
    window = jnp.where(group == 0, 2.0, jnp.where(group == 1, 4.0, jnp.where(group == 2, 8.0, 16.0)))
    place = start[0] + lax.broadcasted_iota(jnp.int32, (rows, LANES), 0)
    counts = jnp.minimum(place.astype(jnp.float32) + 1.0, window)
    inverse = jnp.concatenate([1.0 / counts] * (trail.shape[1] // LANES), axis=1)
    diff = (trail * inverse - wide[first:high, :]).astype(jnp.bfloat16)
    mapped = jnp.dot(diff, mix[0], preferred_element_type=jnp.float32)
    out[0] = (mapped * scale[...]).astype(out.dtype)


def pool_mixed(start, x, mix, scale):
    seqs, total, width = x.shape
    groups, head, _ = mix.shape
    assert groups % 4 == 0
    rows = total - HALO
    return pl.pallas_call(
        pool_kernel,
        out_shape=jax.ShapeDtypeStruct((seqs, rows, width), jnp.bfloat16),
        grid_spec=pltpu.PrefetchScalarGridSpec(
            num_scalar_prefetch=1,
            grid=(seqs, groups),
            in_specs=[
                pl.BlockSpec((1, total, head), lambda i, g, *_: (i, 0, g)),
                pl.BlockSpec((1, head, head), lambda i, g, *_: (g, 0, 0)),
                pl.BlockSpec((1, head), lambda i, g, *_: (0, g)),
            ],
            out_specs=pl.BlockSpec((1, rows, head), lambda i, g, *_: (i, 0, g)),
            scratch_shapes=[pltpu.VMEM((8 + total, head), jnp.float32)] * 4,
        ),
        compiler_params=pltpu.CompilerParams(vmem_limit_bytes=VMEM_LIMIT),
        cost_estimate=pl.CostEstimate(
            flops=4_000_000_000, transcendentals=0, bytes_accessed=4_000_000
        ),
        name="pool_mixed",
    )(start, x, mix, scale.reshape(1, width))


def exit_kernel(chain_places, pool_places, side, h, p, seam_h, seam_p, entering, pooled, *refs):
    count = len(chain_places) + len(pool_places)
    stacks, (out, lhs, held, sems) = refs[:count], refs[count:]
    chain_stacks, pool_stacks = stacks[: len(chain_places)], stacks[len(chain_places) :]
    seqs, half, width = h.shape
    tile = held.shape[2]
    per = tile // LANES

    def copies(j):
        found = []
        for kind, (group, places) in enumerate(
            ((chain_stacks, chain_places), (pool_stacks, pool_places))
        ):
            for stack, places_of in zip(group, places):
                for m, r in enumerate(places_of):
                    if r // per == j:
                        found.append(
                            pltpu.make_async_copy(
                                stack.at[m],
                                held.at[j, pl.ds(kind * width, width), pl.ds((r % per) * LANES, LANES)],
                                sems.at[kind, r],
                            )
                        )
        return found

    tiles = held.shape[0]
    for j in range(tiles):
        for copy in copies(j):
            copy.start()
    span = 2 * half // CHUNKS
    in_half = half // span
    for s in range(seqs):
        for c in range(in_half):
            seam = side[0] * in_half + c
            gone_in = (
                seam_h[s, pl.ds(seam, 1), :] + seam_p[s, pl.ds(seam, 1), :] * entering[s : s + 1, :]
            )
            rows = slice(c * span, (c + 1) * span)
            lhs[s * half + c * span : s * half + (c + 1) * span, 0:width] = (
                h[s, rows, :] + p[s, rows, :] * gone_in
            ).astype(lhs.dtype)
        lhs[s * half : (s + 1) * half, width:] = pooled[s]
    for j in range(tiles):
        for copy in copies(j):
            copy.wait()
        got = jnp.dot(lhs[...], held[j], preferred_element_type=jnp.float32).astype(out.dtype)
        for s in range(seqs):
            out[s, :, j * tile : (j + 1) * tile] = got[s * half : (s + 1) * half]


def exit_dot(side, h, p, seam_h, seam_p, entering, pooled, chain_parts, pool_parts, dtype, name):
    seqs, rows, width = h.shape
    half = rows // 2
    shards = sum(len(q[1]) for q in chain_parts)
    tile = 2 * LANES
    whole = lambda a: pl.BlockSpec(a.shape, lambda i, *_: (0,) * a.ndim)
    part = pl.BlockSpec((seqs, half, width), lambda i, side: (0, side[0], 0))
    parts = chain_parts + pool_parts
    return pl.pallas_call(
        functools.partial(exit_kernel, [q[1] for q in chain_parts], [q[1] for q in pool_parts]),
        out_shape=jax.ShapeDtypeStruct((seqs, half, shards * LANES), dtype),
        grid_spec=pltpu.PrefetchScalarGridSpec(
            num_scalar_prefetch=1,
            grid=(1,),
            in_specs=[part, part, whole(seam_h), whole(seam_p), whole(entering), part]
            + [pl.BlockSpec(memory_space=pl.ANY)] * len(parts),
            out_specs=pl.BlockSpec((seqs, half, shards * LANES), lambda i, *_: (0, 0, 0)),
            scratch_shapes=[
                pltpu.VMEM((seqs * half, 2 * width), jnp.bfloat16),
                pltpu.VMEM((shards * LANES // tile, 2 * width, tile), jnp.bfloat16),
                pltpu.SemaphoreType.DMA((2, shards)),
            ],
        ),
        compiler_params=pltpu.CompilerParams(vmem_limit_bytes=VMEM_LIMIT),
        cost_estimate=pl.CostEstimate(
            flops=4 * seqs * half * width * shards * LANES, transcendentals=0, bytes_accessed=8_000_000
        ),
        name=name,
    )(side, h, p, seam_h, seam_p, entering, pooled, *[q[0] for q in parts])


def merge_kernel(order, mine, came, out):
    for b in range(out.shape[2] // LANES):
        col = pl.multiple_of(order[b] * LANES, LANES)
        cols = slice(b * LANES, (b + 1) * LANES)
        out[0, :, pl.ds(col, LANES)] = (mine[0, :, cols] + came[0, :, cols].astype(jnp.float32)).astype(
            out.dtype
        )


def merge_rows(order, mine, came):
    seqs, half, width = mine.shape
    block = pl.BlockSpec((1, half, width), lambda i, *_: (i, 0, 0))
    return pl.pallas_call(
        merge_kernel,
        out_shape=jax.ShapeDtypeStruct((seqs, half, width), jnp.bfloat16),
        grid_spec=pltpu.PrefetchScalarGridSpec(
            num_scalar_prefetch=1, grid=(seqs,), in_specs=[block, block], out_specs=block
        ),
        compiler_params=pltpu.CompilerParams(vmem_limit_bytes=VMEM_LIMIT),
        name="merge_rows",
    )(order, mine, came)


def weights_and_order(chain_entry, pool_entry, chain_exit, pool_exit, width):
    sp_n, fs_n = lax.axis_size("sp"), lax.axis_size("fs")
    if chain_entry.shape[0] % LANES == 0 and chain_exit.shape[1] == LANES and fs_n == 4:
        go = functools.partial(gather_blocks, sp_n=sp_n, fs_n=fs_n)
        found = (
            go(chain_entry, ROUTES["ce"]),
            go(pool_entry, ROUTES["pe"]),
            go(chain_exit, ROUTES["cx"]),
            go(pool_exit, ROUTES["px"]),
        )
        place, spot = lax.axis_index("sp"), lax.axis_index("fs")
        lap = jnp.arange(sp_n, dtype=jnp.int32)[None, :]
        swap = jnp.arange(fs_n, dtype=jnp.int32)[:, None]
        order = ((place - lap) % sp_n) * fs_n + (spot ^ swap)
        return found, order.reshape(-1).astype(jnp.int32)
    blocks = width // LANES
    places = list(range(blocks))
    entry = lambda w: [
        (lax.all_gather(w, ("sp", "fs"), axis=0, tiled=True).reshape(blocks, -1, w.shape[1]), places)
    ]
    leave = lambda w: [
        (
            lax.all_gather(w, ("sp", "fs"), axis=1, tiled=True)
            .reshape(w.shape[0], blocks, LANES)
            .transpose(1, 0, 2),
            places,
        )
    ]
    found = entry(chain_entry), entry(pool_entry), leave(chain_exit), leave(pool_exit)
    return found, jnp.arange(blocks, dtype=jnp.int32)


def per_device(
    tokens,
    norm_gain,
    chain_entry,
    pool_entry,
    conv_taps,
    recur_gate,
    input_gate,
    decay_log,
    decay_shift,
    start_state,
    pool_mix,
    pool_scale,
    chain_exit,
    pool_exit,
):
    sp_n, tp_n = lax.axis_size("sp"), lax.axis_size("tp")
    assert tp_n == 2
    seqs, half, width = tokens.shape
    rows = half * tp_n
    place, core = lax.axis_index("sp"), lax.axis_index("tp")
    side = jnp.reshape(core, (1,)).astype(jnp.int32)
    other_side = 1 - side
    (ce, pe, cx, px), order = weights_and_order(chain_entry, pool_entry, chain_exit, pool_exit, width)

    swap_tp = [(0, 1), (1, 0)]
    other = lax.ppermute(tokens, "tp", swap_tp)
    tail = jnp.where(core == 1, tokens[:, half - HALO :], other[:, half - HALO :])
    halo = lax.ppermute(tail, "sp", [(i, i + 1) for i in range(sp_n - 1)])
    normed = norm_rows(order, side, tokens, other, halo, norm_gain)
    flat = normed.reshape(seqs * (rows + HALO), width)

    chain_input = entry_dot(flat, ce, "chain_entry").reshape(seqs, rows + HALO, -1)
    pool_input = entry_dot(flat, pe, "pool_entry").reshape(seqs, rows + HALO, -1)

    h, p, seam_h, seam_p = chain_scan(
        chain_input, conv_taps, recur_gate, input_gate, decay_log, decay_shift, rows * sp_n
    )
    last = jnp.stack([seam_p[:, CHUNKS], seam_h[:, CHUNKS]])
    entering = start_state
    for back in range(sp_n - 1, 0, -1):
        came = lax.ppermute(last, "sp", [(i, i + back) for i in range(sp_n - back)])
        entering = jnp.where(place >= back, came[0] * entering + came[1], entering)

    start = jnp.reshape(place * rows, (1,)).astype(jnp.int32)
    pooled = pool_mixed(start, pool_input, pool_mix, pool_scale)

    ex = functools.partial(
        exit_dot,
        h=h,
        p=p,
        seam_h=seam_h,
        seam_p=seam_p,
        entering=entering,
        pooled=pooled,
        chain_parts=cx,
        pool_parts=px,
    )
    away = ex(other_side, dtype=jnp.bfloat16, name="exit_other")
    came = lax.ppermute(away, "tp", swap_tp)
    mine = ex(side, dtype=jnp.float32, name="exit_own")
    return merge_rows(order, mine, came)


def solution(mesh):
    in_specs = (
        P("fs", ("sp", "tp"), None),
        P(),
        P(("sp", "fs"), "tp"),
        P(("sp", "fs"), "tp"),
        P(None, "tp"),
        P("tp", None, None),
        P("tp", None, None),
        P("tp"),
        P("fs", "sp", "tp"),
        P("fs", "tp"),
        P("tp", None, None),
        P("tp"),
        P("tp", ("sp", "fs")),
        P("tp", ("sp", "fs")),
    )
    out_specs = P("fs", ("sp", "tp"), None)
    return jax.shard_map(
        per_device, mesh=mesh, in_specs=in_specs, out_specs=out_specs, check_vma=False
    )
```

```python
import functools

import jax
import jax.numpy as jnp
from jax import lax
from jax.experimental import pallas as pl
from jax.experimental.pallas import tpu as pltpu
from jax.sharding import PartitionSpec as P


HALO = 16
LANES = 128
NORM_EPSILON = 1e-06
RECUR_SCALE = 8.0
CHUNKS = 8
MIB = 1024 * 1024
ROUTES = {"E1": ("xy", "yx", "xy", "yx"), "E2": ("xy", "yx", "xy", "yx"), "X1": "yzx", "X2": "xzy"}
LATE_LAPS = 1


def ring_pairs(size):
    return [(i, (i + 1) % size) for i in range(size)]


def swap_pairs(size, bit):
    return [(i, i ^ bit) for i in range(size)]


def join(values):
    return jnp.concatenate(values, axis=0)


def gather_part(own, route, sp_n, fs_n):
    own = own[None]
    ring = ring_pairs(sp_n)

    def swapped(part, step):
        stack, places = part
        bit = 1 if step == "x" else 2
        came = lax.ppermute(stack, "fs", swap_pairs(fs_n, bit))
        return came, [(f ^ bit, s) for f, s in places]

    found = []
    if isinstance(route, tuple):
        held = (own, [(0, 0)])
        for lap in range(sp_n):
            if lap:
                held = (lax.ppermute(held[0], "sp", ring), [(0, lap)])
            one, two = route[lap % len(route)]
            first = swapped(held, one)
            found += [held, first]
            found += [swapped(held, two), swapped(first, two)]
    elif route[0] == "z":
        one, two = route[1], route[2]
        laps = [own]
        for _ in range(1, sp_n):
            laps.append(lax.ppermute(laps[-1], "sp", ring))
        for group in (range(0, sp_n // 2), range(sp_n // 2, sp_n)):
            held = join([laps[i] for i in group])
            held = (held, [(0, i) for i in group])
            first = swapped(held, one)
            found += [held, first]
            found += [swapped(held, two), swapped(first, two)]
    else:
        one, two = route[0], route[2]
        first = swapped((own, [(0, 0)]), one)
        held = (join([own, first[0]]), [(0, 0)] + first[1])
        for lap in range(sp_n):
            if lap:
                stack = lax.ppermute(held[0], "sp", ring)
                held = (stack, [(f, lap) for f, _ in held[1]])
            found += [held, swapped(held, two)]
    return [(stack, [f * sp_n + s for f, s in places]) for stack, places in found]


def norm_kernel(order, side, own, other, halo, gain, out):
    blocks = own.shape[2] // LANES
    half = own.shape[1]
    width = own.shape[2]

    def rows_of(src, base, count, size):
        def one(i, _):
            at = pl.multiple_of(i * size, size)
            squares = None
            for b in range(blocks):
                part = src[0, pl.ds(at, size), b * LANES : (b + 1) * LANES].astype(jnp.float32)
                squares = part * part if squares is None else squares + part * part
            mean = jnp.sum(squares, axis=-1, keepdims=True) * (1.0 / width)
            scale = jnp.broadcast_to(lax.rsqrt(mean + NORM_EPSILON), (size, LANES))
            to = pl.multiple_of(base + i * size, HALO)
            for b in range(blocks):
                col = pl.multiple_of(order[b] * LANES, LANES)
                part = src[0, pl.ds(at, size), pl.ds(col, LANES)].astype(jnp.float32)
                out[0, pl.ds(to, size), b * LANES : (b + 1) * LANES] = (
                    part * scale * gain[:, pl.ds(col, LANES)]
                ).astype(out.dtype)
            return 0

        lax.fori_loop(0, count, one, 0)

    size = 64 if half % 64 == 0 else HALO
    rows_of(halo, 0, 1, HALO)
    rows_of(own, HALO + side[0] * half, half // size, size)
    rows_of(other, HALO + (1 - side[0]) * half, half // size, size)


def norm_rows(order, side, own, other, halo, gain):
    seqs, half, width = own.shape
    rows = 2 * half + HALO
    return pl.pallas_call(
        norm_kernel,
        out_shape=jax.ShapeDtypeStruct((seqs, rows, width), jnp.bfloat16),
        grid_spec=pltpu.PrefetchScalarGridSpec(
            num_scalar_prefetch=2,
            grid=(seqs,),
            in_specs=[
                pl.BlockSpec((1, half, width), lambda i, *_: (i, 0, 0)),
                pl.BlockSpec((1, half, width), lambda i, *_: (i, 0, 0)),
                pl.BlockSpec((1, HALO, width), lambda i, *_: (i, 0, 0)),
                pl.BlockSpec((1, width), lambda i, *_: (0, 0)),
            ],
            out_specs=pl.BlockSpec((1, rows, width), lambda i, *_: (i, 0, 0)),
        ),
        compiler_params=pltpu.CompilerParams(vmem_limit_bytes=24 * MIB),
        cost_estimate=pl.CostEstimate(flops=4_000_000_000, transcendentals=0, bytes_accessed=8_000_000),
        name="norm_rows",
    )(order, side, own, other, halo, gain.reshape(1, width))


def entry_kernel(places, seqs, x, *refs):
    stacks, (out, held, sems) = refs[: len(places)], refs[len(places) :]
    depth = stacks[0].shape[1]
    tiles, _, tile = held.shape
    rows = x.shape[0] // seqs

    def copies(j):
        return [
            pltpu.make_async_copy(
                stack.at[m, :, pl.ds(j * tile, tile)],
                held.at[j, pl.ds(r * depth, depth), :],
                sems.at[j, r],
            )
            for stack, places_of in zip(stacks, places)
            for m, r in enumerate(places_of)
        ]

    for j in range(tiles):
        for copy in copies(j):
            copy.start()
    for j in range(tiles):
        for copy in copies(j):
            copy.wait()
        for s in range(seqs):
            out[s * rows : (s + 1) * rows, j * tile : (j + 1) * tile] = jnp.dot(
                x[s * rows : (s + 1) * rows, :], held[j], preferred_element_type=jnp.float32
            ).astype(out.dtype)


def entry_dot(x, parts):
    seqs, total, depth = x.shape
    rows = seqs * total
    width = parts[0][0].shape[2]
    tile = min(2 * LANES, width)
    shards = depth // parts[0][0].shape[1]
    return pl.pallas_call(
        functools.partial(entry_kernel, [places for _, places in parts], seqs),
        out_shape=jax.ShapeDtypeStruct((rows, width), jnp.bfloat16),
        in_specs=[pl.BlockSpec(memory_space=pltpu.VMEM)]
        + [pl.BlockSpec(memory_space=pl.ANY)] * len(parts),
        out_specs=pl.BlockSpec(memory_space=pltpu.VMEM),
        scratch_shapes=[
            pltpu.VMEM((width // tile, depth, tile), jnp.bfloat16),
            pltpu.SemaphoreType.DMA((width // tile, shards)),
        ],
        compiler_params=pltpu.CompilerParams(vmem_limit_bytes=20 * MIB),
        cost_estimate=pl.CostEstimate(
            flops=2 * rows * depth * width, transcendentals=0, bytes_accessed=2 * depth * width
        ),
    )(x.reshape(rows, depth), *[stack for stack, _ in parts]).reshape(seqs, total, width)


def chain_kernel(length, x, taps, wr, wi, rate_log, shift, h_out, p_out, seam_h, seam_p, wide):
    rows = shift.shape[1]
    span = rows // CHUNKS
    tap_count = taps.shape[0]
    wide[...] = x[0].astype(jnp.float32)
    first = HALO - (tap_count - 1)
    conv = wide[first : first + rows, :] * taps[0:1, :].astype(jnp.float32)
    for j in range(1, tap_count):
        conv = conv + wide[first + j : first + j + rows, :] * taps[j : j + 1, :].astype(jnp.float32)
    conv = conv.astype(jnp.bfloat16)
    to_recur = jnp.dot(conv, wr[0], preferred_element_type=jnp.float32)
    to_input = jnp.dot(conv, wi[0], preferred_element_type=jnp.float32)
    gate_recur = 0.5 * jnp.tanh(0.5 * to_recur) + 0.5
    gate_input = 0.5 * jnp.tanh(0.5 * to_input) + 0.5
    rate = jnp.exp(rate_log[...]) * (-RECUR_SCALE / length)
    log_decay = gate_recur * rate + shift[0]
    decay = jnp.exp(log_decay)
    twice = 2.0 * log_decay
    series = 1.0 + twice * (1.0 / 8.0)
    for k in range(7, 1, -1):
        series = 1.0 + twice * (1.0 / k) * series
    gone = jnp.where(twice > -0.5, -twice * series, 1.0 - decay * decay)
    root = gone * lax.rsqrt(jnp.maximum(gone, 1e-37))
    drive = root * gate_input * conv.astype(jnp.float32)
    width = wide.shape[1]
    lanes = [slice(b * LANES, (b + 1) * LANES) for b in range(width // LANES)]
    for b, cols in enumerate(lanes):
        p_out[0, b] = decay[:, cols]
        h_out[0, b] = drive[:, cols]
    states = [jnp.zeros((CHUNKS, LANES), jnp.float32) for _ in lanes]
    keeps = [jnp.ones((CHUNKS, LANES), jnp.float32) for _ in lanes]
    for t in range(span):
        step = pl.ds(t, CHUNKS, stride=span)
        for b in range(len(lanes)):
            a = p_out[0, b, step, :]
            states[b] = a * states[b] + h_out[0, b, step, :]
            keeps[b] = a * keeps[b]
            h_out[0, b, step, :] = states[b]
            p_out[0, b, step, :] = keeps[b]
    state = jnp.concatenate(states, axis=1)
    kept = jnp.concatenate(keeps, axis=1)
    before_h = jnp.zeros((1, width), jnp.float32)
    before_p = jnp.ones((1, width), jnp.float32)
    for c in range(CHUNKS):
        seam_h[0, c : c + 1, :] = before_h
        seam_p[0, c : c + 1, :] = before_p
        before_h = kept[c : c + 1] * before_h + state[c : c + 1]
        before_p = kept[c : c + 1] * before_p
    seam_h[0, CHUNKS : 2 * CHUNKS, :] = jnp.broadcast_to(before_h, (CHUNKS, width))
    seam_p[0, CHUNKS : 2 * CHUNKS, :] = jnp.broadcast_to(before_p, (CHUNKS, width))


def chain_scan(x, taps, wr, wi, rate_log, shift, length):
    seqs, rows, width = shift.shape
    heads, head, _ = wr.shape
    return pl.pallas_call(
        functools.partial(chain_kernel, length),
        out_shape=(
            jax.ShapeDtypeStruct((seqs, width // LANES, rows, LANES), jnp.float32),
            jax.ShapeDtypeStruct((seqs, width // LANES, rows, LANES), jnp.float32),
            jax.ShapeDtypeStruct((seqs, 2 * CHUNKS, width), jnp.float32),
            jax.ShapeDtypeStruct((seqs, 2 * CHUNKS, width), jnp.float32),
        ),
        grid=(seqs, heads),
        in_specs=[
            pl.BlockSpec((1, rows + HALO, head), lambda i, g: (i, 0, g)),
            pl.BlockSpec((taps.shape[0], head), lambda i, g: (0, g)),
            pl.BlockSpec((1, head, head), lambda i, g: (g, 0, 0)),
            pl.BlockSpec((1, head, head), lambda i, g: (g, 0, 0)),
            pl.BlockSpec((1, head), lambda i, g: (0, g)),
            pl.BlockSpec((1, rows, head), lambda i, g: (i, 0, g)),
        ],
        out_specs=(
            pl.BlockSpec((1, head // LANES, rows, LANES), lambda i, g: (i, g, 0, 0)),
            pl.BlockSpec((1, head // LANES, rows, LANES), lambda i, g: (i, g, 0, 0)),
            pl.BlockSpec((1, 2 * CHUNKS, head), lambda i, g: (i, 0, g)),
            pl.BlockSpec((1, 2 * CHUNKS, head), lambda i, g: (i, 0, g)),
        ),
        scratch_shapes=[pltpu.VMEM((rows + HALO, head), jnp.float32)],
        compiler_params=pltpu.CompilerParams(vmem_limit_bytes=24 * MIB),
        cost_estimate=pl.CostEstimate(
            flops=8_000_000_000, transcendentals=0, bytes_accessed=12_000_000
        ),
        name="chain_scan",
    )(x, taps, wr, wi, rate_log.reshape(1, width), shift)


def pool_kernel(start, x, mix, scale, out, wide, sums):
    rows = out.shape[1]
    total = rows + HALO
    low, high = 8, 8 + total
    first = low + HALO
    group = lax.rem(pl.program_id(1), 4)
    width = wide.shape[1]
    wide[0:low, :] = jnp.zeros((low, width), jnp.float32)
    wide[low:high, :] = x[0].astype(jnp.float32)

    def finish(trail, window):
        place = start[0] + lax.broadcasted_iota(jnp.int32, (rows, LANES), 0)
        counts = jnp.minimum(place.astype(jnp.float32) + 1.0, window)
        inverse = jnp.concatenate([1.0 / counts] * (width // LANES), axis=1)
        diff = (trail * inverse - wide[first:high, :]).astype(jnp.bfloat16)
        mapped = jnp.dot(diff, mix[0], preferred_element_type=jnp.float32)
        out[0] = (mapped * scale[...]).astype(out.dtype)

    for depth in range(4):

        @pl.when(group == depth)
        def _(depth=depth):
            held = wide
            for level in range(depth):
                reach = 2**level
                sums[level, 0:low, :] = jnp.zeros((low, width), jnp.float32)
                sums[level, low:high, :] = held[low:high, :] + held[low - reach : high - reach, :]
                held = sums.at[level]
            reach = 2**depth
            finish(held[first:high, :] + held[first - reach : high - reach, :], 2.0 * reach)


def pool_mixed(start, x, mix, scale):
    seqs, total, width = x.shape
    groups, head, _ = mix.shape
    assert groups % 4 == 0
    rows = total - HALO
    return pl.pallas_call(
        pool_kernel,
        out_shape=jax.ShapeDtypeStruct((seqs, rows, width), jnp.bfloat16),
        grid_spec=pltpu.PrefetchScalarGridSpec(
            num_scalar_prefetch=1,
            grid=(seqs, groups),
            in_specs=[
                pl.BlockSpec((1, total, head), lambda i, g, *_: (i, 0, g)),
                pl.BlockSpec((1, head, head), lambda i, g, *_: (g, 0, 0)),
                pl.BlockSpec((1, head), lambda i, g, *_: (0, g)),
            ],
            out_specs=pl.BlockSpec((1, rows, head), lambda i, g, *_: (i, 0, g)),
            scratch_shapes=[
                pltpu.VMEM((8 + total, head), jnp.float32),
                pltpu.VMEM((3, 8 + total, head), jnp.float32),
            ],
        ),
        compiler_params=pltpu.CompilerParams(vmem_limit_bytes=24 * MIB),
        cost_estimate=pl.CostEstimate(
            flops=4_000_000_000, transcendentals=0, bytes_accessed=4_000_000
        ),
        name="pool_mixed",
    )(start, x, mix, scale.reshape(1, width))


def recurrent_kernel(h, p, seam_h, seam_p, entering, out):
    seqs, blocks, rows, _ = h.shape
    span = rows // CHUNKS
    for s in range(seqs):
        for b in range(blocks):
            cols = slice(b * LANES, (b + 1) * LANES)
            for c in range(CHUNKS):
                one = slice(c, c + 1)
                gone_in = seam_h[s, one, cols] + seam_p[s, one, cols] * entering[s : s + 1, cols]
                at = slice(c * span, (c + 1) * span)
                out[s, at, cols] = (h[s, b, at, :] + p[s, b, at, :] * gone_in).astype(out.dtype)


def recurrent_rows(h, p, seam_h, seam_p, entering):
    seqs, blocks, rows, _ = h.shape
    vmem = pl.BlockSpec(memory_space=pltpu.VMEM)
    return pl.pallas_call(
        recurrent_kernel,
        out_shape=jax.ShapeDtypeStruct((seqs, rows, blocks * LANES), jnp.bfloat16),
        in_specs=[vmem] * 5,
        out_specs=vmem,
        compiler_params=pltpu.CompilerParams(vmem_limit_bytes=16 * MIB),
        cost_estimate=pl.CostEstimate(
            flops=2_000_000_000, transcendentals=0, bytes_accessed=8_000_000
        ),
    )(h, p, seam_h, seam_p, entering)


def exit_kernel(chain_spots, pool_spots, counts, shards, merged, *refs):
    if merged:
        order, side, recurrent, pooled, came, *refs = refs
    else:
        side, recurrent, pooled, *refs = refs
    chain_stacks, pool_stacks = refs[: counts[0]], refs[counts[0] : sum(counts)]
    refs = refs[sum(counts) :]
    if merged:
        out, held, sem = refs[-3:]
    else:
        (out,) = refs
    seqs, rows, _ = recurrent.shape
    half = rows // 2
    at = pl.ds(pl.multiple_of(side[0] * half, half), half)
    left = jnp.concatenate([recurrent[s, at, :] for s in range(seqs)], axis=0)
    left_pool = jnp.concatenate([pooled[s, at, :] for s in range(seqs)], axis=0)

    def columns(stacks, spots, pair):
        found = []
        for i in pair:
            stack, m = spots[shards[i]]
            found.append(stacks[stack][m])
        return jnp.concatenate(found, axis=1)

    copies = []
    for j in range(0, len(shards), 2):
        pair = range(j, min(j + 2, len(shards)))
        got = jnp.dot(
            left, columns(chain_stacks, chain_spots, pair), preferred_element_type=jnp.float32
        ) + jnp.dot(
            left_pool, columns(pool_stacks, pool_spots, pair), preferred_element_type=jnp.float32
        )
        cols = slice(j * LANES, (j + len(pair)) * LANES)
        for s in range(seqs):
            rows_of = got[s * half : (s + 1) * half]
            if merged:
                rows_of = rows_of + came[s, :, cols].astype(jnp.float32)
                held[s, :, cols] = rows_of.astype(out.dtype)
            else:
                out[s, :, cols] = rows_of.astype(out.dtype)
        if merged:
            for i in pair:
                to = pl.multiple_of(order[shards[i]] * LANES, LANES)
                copies.append(
                    pltpu.make_async_copy(
                        held.at[:, :, i * LANES : (i + 1) * LANES],
                        out.at[:, :, pl.ds(to, LANES)],
                        sem.at[i],
                    )
                )
                copies[-1].start()
    for copy in copies:
        copy.wait()


def exit_columns(side, recurrent, pooled, chain_parts, pool_parts, shards, merge=None):
    seqs, rows, width = recurrent.shape
    half = rows // 2
    wide = len(shards) * LANES

    def used(parts):
        kept = [q for q in parts if any(r in shards for r in q[1])]
        return [q[0] for q in kept], {r: (i, m) for i, q in enumerate(kept) for m, r in enumerate(q[1])}

    chain_stacks, chain_spots = used(chain_parts)
    pool_stacks, pool_spots = used(pool_parts)
    counts = (len(chain_stacks), len(pool_stacks))
    vmem = pl.BlockSpec(memory_space=pltpu.VMEM)
    smem = pl.BlockSpec(memory_space=pltpu.SMEM)
    stacks = (*chain_stacks, *pool_stacks)
    if merge is None:
        args = (side, recurrent, pooled, *stacks)
        specs = [smem] + [vmem] * (len(args) - 1)
        out_shape = jax.ShapeDtypeStruct((seqs, half, wide), jnp.bfloat16)
        extra = dict(out_specs=vmem)
    else:
        order, came, result = merge
        args = (order, side, recurrent, pooled, came, *stacks)
        specs = [smem, smem] + [vmem] * (len(args) - 2)
        aliases = {}
        if result is not None:
            args, specs = (*args, result), specs + [pl.BlockSpec(memory_space=pl.ANY)]
            aliases = {len(args) - 1: 0}
        out_shape = jax.ShapeDtypeStruct((seqs, half, order.shape[0] * LANES), jnp.bfloat16)
        extra = dict(
            out_specs=pl.BlockSpec(memory_space=pl.ANY),
            input_output_aliases=aliases,
            scratch_shapes=[
                pltpu.VMEM((seqs, half, wide), jnp.bfloat16),
                pltpu.SemaphoreType.DMA((len(shards),)),
            ],
        )
    return pl.pallas_call(
        functools.partial(exit_kernel, chain_spots, pool_spots, counts, shards, merge is not None),
        out_shape=out_shape,
        in_specs=specs,
        compiler_params=pltpu.CompilerParams(vmem_limit_bytes=32 * MIB),
        cost_estimate=pl.CostEstimate(
            flops=4 * seqs * half * width * wide, transcendentals=0, bytes_accessed=6_000_000
        ),
        **extra,
    )(*args)


def weights_and_order(chain_entry, pool_entry, chain_exit, pool_exit, width):
    sp_n, fs_n = lax.axis_size("sp"), lax.axis_size("fs")
    if chain_entry.shape[0] % LANES == 0 and chain_exit.shape[1] == LANES and fs_n == 4:
        go = lambda own, name: gather_part(own, ROUTES[name], sp_n, fs_n)
        found = go(chain_entry, "E1"), go(pool_entry, "E2"), go(chain_exit, "X1"), go(pool_exit, "X2")
        place, spot = lax.axis_index("sp"), lax.axis_index("fs")
        lap = jnp.arange(sp_n, dtype=jnp.int32)[None, :]
        swap = jnp.arange(fs_n, dtype=jnp.int32)[:, None]
        order = ((place - lap) % sp_n) * fs_n + (spot ^ swap)
        return found, order.reshape(-1).astype(jnp.int32)
    blocks = width // LANES
    places = list(range(blocks))
    entry = lambda w: [
        (lax.all_gather(w, ("sp", "fs"), axis=0, tiled=True).reshape(blocks, -1, w.shape[1]), places)
    ]
    leave = lambda w: [
        (
            lax.all_gather(w, ("sp", "fs"), axis=1, tiled=True)
            .reshape(w.shape[0], blocks, LANES)
            .transpose(1, 0, 2),
            places,
        )
    ]
    found = entry(chain_entry), entry(pool_entry), leave(chain_exit), leave(pool_exit)
    return found, jnp.arange(blocks, dtype=jnp.int32)


def per_device(
    tokens,
    norm_gain,
    chain_entry,
    pool_entry,
    conv_taps,
    recur_gate,
    input_gate,
    decay_log,
    decay_shift,
    start_state,
    pool_mix,
    pool_scale,
    chain_exit,
    pool_exit,
):
    sp_n, tp_n = lax.axis_size("sp"), lax.axis_size("tp")
    assert tp_n == 2
    _, half, width = tokens.shape
    rows = half * tp_n
    place, core = lax.axis_index("sp"), lax.axis_index("tp")
    side = jnp.reshape(core, (1,)).astype(jnp.int32)
    other_side = 1 - side
    (ce, pe, cx, px), order = weights_and_order(chain_entry, pool_entry, chain_exit, pool_exit, width)

    swap_tp = [(0, 1), (1, 0)]
    other = lax.ppermute(tokens, "tp", swap_tp)
    tail = jnp.where(core == 1, tokens[:, half - HALO :], other[:, half - HALO :])
    halo = lax.ppermute(tail, "sp", [(i, i + 1) for i in range(sp_n - 1)])
    normed = norm_rows(order, side, tokens, other, halo, norm_gain)

    chain_input = entry_dot(normed, ce)
    pool_input = entry_dot(normed, pe)

    h, p, seam_h, seam_p = chain_scan(
        chain_input, conv_taps, recur_gate, input_gate, decay_log, decay_shift, rows * sp_n
    )
    last = jnp.stack([seam_p[:, CHUNKS], seam_h[:, CHUNKS]])
    entering = start_state
    for back in range(sp_n - 1, 0, -1):
        came = lax.ppermute(last, "sp", [(i, i + back) for i in range(sp_n - back)])
        entering = jnp.where(place >= back, came[0] * entering + came[1], entering)

    start = jnp.reshape(place * rows, (1,)).astype(jnp.int32)
    pooled = pool_mixed(start, pool_input, pool_mix, pool_scale)

    recurrent = recurrent_rows(h, p, seam_h, seam_p, entering)

    count = order.shape[0]
    laps = sp_n if count % sp_n == 0 else count
    late = tuple(r for r in range(count) if r % laps >= laps - LATE_LAPS)
    early = tuple(r for r in range(count) if r % laps < laps - LATE_LAPS)
    ex = lambda at, shards, merge=None: exit_columns(at, recurrent, pooled, cx, px, shards, merge)
    came_early = lax.ppermute(ex(other_side, early), "tp", swap_tp)
    came_late = lax.ppermute(ex(other_side, late), "tp", swap_tp)
    result = ex(side, early, (order, came_early, None))
    return ex(side, late, (order, came_late, result))


def solution(mesh):
    in_specs = (
        P("fs", ("sp", "tp"), None),
        P(),
        P(("sp", "fs"), "tp"),
        P(("sp", "fs"), "tp"),
        P(None, "tp"),
        P("tp", None, None),
        P("tp", None, None),
        P("tp"),
        P("fs", "sp", "tp"),
        P("fs", "tp"),
        P("tp", None, None),
        P("tp"),
        P("tp", ("sp", "fs")),
        P("tp", ("sp", "fs")),
    )
    out_specs = P("fs", ("sp", "tp"), None)

    return jax.shard_map(per_device, mesh=mesh, in_specs=in_specs, out_specs=out_specs, check_vma=False)
```

```python
import functools

import jax
import jax.numpy as jnp
from jax import lax
from jax.experimental import pallas as pl
from jax.experimental.pallas import tpu as pltpu
from jax.sharding import PartitionSpec as P


HALO = 16
LANES = 128
NORM_EPSILON = 1e-06
RECUR_SCALE = 8.0
CHUNKS = 8
MIB = 1024 * 1024
ROUTES = {"E1": ("xyx", "xyy", "xyx", "xyy"), "E2": ("xyx", "xyy", "xyx", "xyy"), "X1": "yzx", "X2": "xzy"}
LATE_LAPS = 1


def ring_pairs(size):
    return [(i, (i + 1) % size) for i in range(size)]


def swap_pairs(size, bit):
    return [(i, i ^ bit) for i in range(size)]


def join(values):
    return jnp.concatenate(values, axis=0)


def gather_part(own, route, sp_n, fs_n):
    own = own[None]
    ring = ring_pairs(sp_n)

    def swapped(part, step):
        stack, places = part
        bit = 1 if step == "x" else 2
        came = lax.ppermute(stack, "fs", swap_pairs(fs_n, bit))
        return came, [(f ^ bit, s) for f, s in places]

    found = []
    if isinstance(route, tuple):
        past = None
        for lap in range(sp_n):
            from_x, from_y, from_both = route[lap % len(route)]

            def along(step, near, kind):
                if step == "z":
                    stack = lax.ppermute(past[kind][0], "sp", ring)
                    return stack, [(f, lap) for f, _ in past[kind][1]]
                return swapped(near, step)

            held = (own, [(0, 0)])
            if lap:
                held = (lax.ppermute(past[0][0], "sp", ring), [(0, lap)])
            over_x = along(from_x, held, 1)
            over_y = along(from_y, held, 2)
            both = along(from_both, over_y if from_both == "x" else over_x, 3)
            past = [held, over_x, over_y, both]
            found += past
    elif route[0] == "z":
        one, two = route[1], route[2]
        laps = [own]
        for lap in range(1, sp_n):
            laps.append(lax.ppermute(laps[-1], "sp", ring))
        for group in (range(0, sp_n // 2), range(sp_n // 2, sp_n)):
            held = join([laps[i] for i in group])
            held = (held, [(0, i) for i in group])
            first = swapped(held, one)
            found += [held, first]
            found += [swapped(held, two), swapped(first, two)]
    else:
        one, two = route[0], route[2]
        first = swapped((own, [(0, 0)]), one)
        held = (join([own, first[0]]), [(0, 0)] + first[1])
        for lap in range(sp_n):
            if lap:
                stack = lax.ppermute(held[0], "sp", ring)
                held = (stack, [(f, lap) for f, _ in held[1]])
            found += [held, swapped(held, two)]
    return [(stack, [f * sp_n + s for f, s in places]) for stack, places in found]


def norm_kernel(order, spot, own, other, halo, gain, out):
    blocks = own.shape[2] // LANES
    half = own.shape[1]
    width = own.shape[2]

    def rows_of(src, base, count, size, keep=None):
        def one(i, _):
            at = pl.multiple_of(i * size, size)
            squares = None
            for b in range(blocks):
                part = src[0, pl.ds(at, size), b * LANES : (b + 1) * LANES].astype(jnp.float32)
                squares = part * part if squares is None else squares + part * part
            mean = jnp.sum(squares, axis=-1, keepdims=True) * (1.0 / width)
            scale = lax.rsqrt(mean + NORM_EPSILON)
            if keep is not None:
                scale = scale * keep
            scale = jnp.broadcast_to(scale, (size, LANES))
            to = pl.multiple_of(base + i * size, HALO)
            for b in range(blocks):
                col = pl.multiple_of(order[b] * LANES, LANES)
                part = src[0, pl.ds(at, size), pl.ds(col, LANES)].astype(jnp.float32)
                out[0, pl.ds(to, size), b * LANES : (b + 1) * LANES] = (
                    part * scale * gain[:, pl.ds(col, LANES)]
                ).astype(out.dtype)
            return 0

        lax.fori_loop(0, count, one, 0)

    size = 64 if half % 64 == 0 else HALO
    rows_of(halo, 0, 1, HALO, jnp.where(spot[1] > 0, 1.0, 0.0))
    rows_of(own, HALO + spot[0] * half, half // size, size)
    rows_of(other, HALO + (1 - spot[0]) * half, half // size, size)


def norm_rows(order, spot, own, other, halo, gain):
    seqs, half, width = own.shape
    rows = 2 * half + HALO
    return pl.pallas_call(
        norm_kernel,
        out_shape=jax.ShapeDtypeStruct((seqs, rows, width), jnp.bfloat16),
        grid_spec=pltpu.PrefetchScalarGridSpec(
            num_scalar_prefetch=2,
            grid=(seqs,),
            in_specs=[
                pl.BlockSpec((1, half, width), lambda i, *_: (i, 0, 0)),
                pl.BlockSpec((1, half, width), lambda i, *_: (i, 0, 0)),
                pl.BlockSpec((1, HALO, width), lambda i, *_: (i, 0, 0)),
                pl.BlockSpec((1, width), lambda i, *_: (0, 0)),
            ],
            out_specs=pl.BlockSpec((1, rows, width), lambda i, *_: (i, 0, 0)),
        ),
        compiler_params=pltpu.CompilerParams(vmem_limit_bytes=12 * MIB),
        cost_estimate=pl.CostEstimate(flops=4_000_000_000, transcendentals=0, bytes_accessed=8_000_000),
        name="norm_rows",
    )(order, spot, own, other, halo, gain.reshape(1, width))


def entry_kernel(places, seqs, x, *refs):
    stacks, (out, held, sems) = refs[: len(places)], refs[len(places) :]
    depth = stacks[0].shape[1]
    tiles, _, tile = held.shape
    rows = x.shape[0] // seqs

    def copies(j):
        return [
            pltpu.make_async_copy(
                stack.at[m, :, pl.ds(j * tile, tile)],
                held.at[j, pl.ds(r * depth, depth), :],
                sems.at[j, r],
            )
            for stack, places_of in zip(stacks, places)
            for m, r in enumerate(places_of)
        ]

    for j in range(tiles):
        for copy in copies(j):
            copy.start()
    for j in range(tiles):
        for copy in copies(j):
            copy.wait()
        for s in range(seqs):
            out[s * rows : (s + 1) * rows, j * tile : (j + 1) * tile] = jnp.dot(
                x[s * rows : (s + 1) * rows, :], held[j], preferred_element_type=jnp.float32
            ).astype(out.dtype)


def entry_dot(x, parts):
    seqs, total, depth = x.shape
    rows = seqs * total
    width = parts[0][0].shape[2]
    tile = min(2 * LANES, width)
    shards = depth // parts[0][0].shape[1]
    return pl.pallas_call(
        functools.partial(entry_kernel, [places for _, places in parts], seqs),
        out_shape=jax.ShapeDtypeStruct((rows, width), jnp.bfloat16),
        in_specs=[pl.BlockSpec(memory_space=pltpu.VMEM)]
        + [pl.BlockSpec(memory_space=pl.ANY)] * len(parts),
        out_specs=pl.BlockSpec(memory_space=pltpu.VMEM),
        scratch_shapes=[
            pltpu.VMEM((width // tile, depth, tile), jnp.bfloat16),
            pltpu.SemaphoreType.DMA((width // tile, shards)),
        ],
        compiler_params=pltpu.CompilerParams(vmem_limit_bytes=14 * MIB),
        cost_estimate=pl.CostEstimate(
            flops=2 * rows * depth * width, transcendentals=0, bytes_accessed=2 * depth * width
        ),
    )(x.reshape(rows, depth), *[stack for stack, _ in parts]).reshape(seqs, total, width)


def chain_kernel(
    length, x, taps, wr, wi, rate_log, shift, h_out, p_out, seam_h, seam_p, wide, conv_at, to_recur, to_input
):
    rows = shift.shape[1]
    span = rows // CHUNKS
    width = wide.shape[1]
    tap_count = taps.shape[0]
    first = HALO - (tap_count - 1)
    lanes = [slice(b * LANES, (b + 1) * LANES) for b in range(width // LANES)]
    wide[...] = x[0].astype(jnp.float32)
    tap = [taps[j : j + 1, :].astype(jnp.float32) for j in range(tap_count)]
    step_rows = 64 if rows % 64 == 0 else rows
    for i in range(rows // step_rows):
        low = i * step_rows
        conv = wide[first + low : first + low + step_rows, :] * tap[0]
        for j in range(1, tap_count):
            conv = conv + wide[first + low + j : first + low + j + step_rows, :] * tap[j]
        conv_at[low : low + step_rows, :] = conv.astype(jnp.bfloat16)
    to_recur[...] = jnp.dot(conv_at[...], wr[0], preferred_element_type=jnp.float32)
    to_input[...] = jnp.dot(conv_at[...], wi[0], preferred_element_type=jnp.float32)
    rate = jnp.exp(rate_log[...]) * (-RECUR_SCALE / length)
    half_rate = 0.5 * rate
    for b, cols in enumerate(lanes):

        def gates(i, _, b=b, cols=cols):
            at = pl.ds(pl.multiple_of(i * step_rows, step_rows), step_rows)
            log_decay = jnp.tanh(0.5 * to_recur[at, cols]) * half_rate[:, cols] + (
                half_rate[:, cols] + shift[0, at, cols]
            )
            decay = jnp.exp(log_decay)
            gone = jnp.tanh(-log_decay) * (1.0 + decay * decay)
            root = gone * lax.rsqrt(jnp.maximum(gone, 1e-37))
            gate_input = 0.5 * jnp.tanh(0.5 * to_input[at, cols]) + 0.5
            p_out[0, b, at, :] = decay
            h_out[0, b, at, :] = root * gate_input * conv_at[at, cols].astype(jnp.float32)
            return 0

        lax.fori_loop(0, rows // step_rows, gates, 0, unroll=2)
    states = [jnp.zeros((CHUNKS, LANES), jnp.float32) for _ in lanes]
    keeps = [jnp.ones((CHUNKS, LANES), jnp.float32) for _ in lanes]
    for t in range(span):
        step = pl.ds(t, CHUNKS, stride=span)
        for b in range(len(lanes)):
            a = p_out[0, b, step, :]
            states[b] = a * states[b] + h_out[0, b, step, :]
            keeps[b] = a * keeps[b]
            h_out[0, b, step, :] = states[b]
            p_out[0, b, step, :] = keeps[b]
    state = jnp.concatenate(states, axis=1)
    kept = jnp.concatenate(keeps, axis=1)
    before_h = jnp.zeros((1, width), jnp.float32)
    before_p = jnp.ones((1, width), jnp.float32)
    for c in range(CHUNKS):
        seam_h[0, c : c + 1, :] = before_h
        seam_p[0, c : c + 1, :] = before_p
        before_h = kept[c : c + 1] * before_h + state[c : c + 1]
        before_p = kept[c : c + 1] * before_p
    seam_h[0, CHUNKS : 2 * CHUNKS, :] = jnp.broadcast_to(before_h, (CHUNKS, width))
    seam_p[0, CHUNKS : 2 * CHUNKS, :] = jnp.broadcast_to(before_p, (CHUNKS, width))


def chain_scan(x, taps, wr, wi, rate_log, shift, length):
    seqs, rows, width = shift.shape
    heads, head, _ = wr.shape
    return pl.pallas_call(
        functools.partial(chain_kernel, length),
        out_shape=(
            pltpu.HBM((seqs, width // LANES, rows, LANES), jnp.float32),
            pltpu.HBM((seqs, width // LANES, rows, LANES), jnp.float32),
            jax.ShapeDtypeStruct((seqs, 2 * CHUNKS, width), jnp.float32),
            jax.ShapeDtypeStruct((seqs, 2 * CHUNKS, width), jnp.float32),
        ),
        grid=(seqs, heads),
        in_specs=[
            pl.BlockSpec((1, rows + HALO, head), lambda i, g: (i, 0, g)),
            pl.BlockSpec((taps.shape[0], head), lambda i, g: (0, g)),
            pl.BlockSpec((1, head, head), lambda i, g: (g, 0, 0)),
            pl.BlockSpec((1, head, head), lambda i, g: (g, 0, 0)),
            pl.BlockSpec((1, head), lambda i, g: (0, g)),
            pl.BlockSpec((1, rows, head), lambda i, g: (i, 0, g)),
        ],
        out_specs=(
            pl.BlockSpec((1, head // LANES, rows, LANES), lambda i, g: (i, g, 0, 0)),
            pl.BlockSpec((1, head // LANES, rows, LANES), lambda i, g: (i, g, 0, 0)),
            pl.BlockSpec((1, 2 * CHUNKS, head), lambda i, g: (i, 0, g)),
            pl.BlockSpec((1, 2 * CHUNKS, head), lambda i, g: (i, 0, g)),
        ),
        scratch_shapes=[
            pltpu.VMEM((rows + HALO, head), jnp.float32),
            pltpu.VMEM((rows, head), jnp.bfloat16),
            pltpu.VMEM((rows, head), jnp.float32),
            pltpu.VMEM((rows, head), jnp.float32),
        ],
        compiler_params=pltpu.CompilerParams(vmem_limit_bytes=10 * MIB),
        cost_estimate=pl.CostEstimate(
            flops=8_000_000_000, transcendentals=0, bytes_accessed=12_000_000
        ),
        name="chain_scan",
    )(x, taps, wr, wi, rate_log.reshape(1, width), shift)


def pool_kernel(start, x, mix, scale, out, wide, sums):
    rows = out.shape[1]
    total = rows + HALO
    low, high = 8, 8 + total
    first = low + HALO
    group = lax.rem(pl.program_id(1), 4)
    width = wide.shape[1]
    wide[0:low, :] = jnp.zeros((low, width), jnp.float32)
    wide[low:high, :] = x[0].astype(jnp.float32)

    def finish(trail, window):
        place = start[0] + lax.broadcasted_iota(jnp.int32, (rows, LANES), 0)
        counts = jnp.minimum(place.astype(jnp.float32) + 1.0, window)
        inverse = jnp.concatenate([1.0 / counts] * (width // LANES), axis=1)
        diff = (trail * inverse - wide[first:high, :]).astype(jnp.bfloat16)
        mapped = jnp.dot(diff, mix[0], preferred_element_type=jnp.float32)
        out[0] = (mapped * scale[...]).astype(out.dtype)

    for depth in range(4):

        @pl.when(group == depth)
        def _(depth=depth):
            held = wide
            for level in range(depth):
                reach = 2**level
                sums[level, 0:low, :] = jnp.zeros((low, width), jnp.float32)
                sums[level, low:high, :] = held[low:high, :] + held[low - reach : high - reach, :]
                held = sums.at[level]
            reach = 2**depth
            finish(held[first:high, :] + held[first - reach : high - reach, :], 2.0 * reach)


def pool_mixed(start, x, mix, scale):
    seqs, total, width = x.shape
    groups, head, _ = mix.shape
    assert groups % 4 == 0
    rows = total - HALO
    return pl.pallas_call(
        pool_kernel,
        out_shape=jax.ShapeDtypeStruct((seqs, rows, width), jnp.bfloat16),
        grid_spec=pltpu.PrefetchScalarGridSpec(
            num_scalar_prefetch=1,
            grid=(seqs, groups),
            in_specs=[
                pl.BlockSpec((1, total, head), lambda i, g, *_: (i, 0, g)),
                pl.BlockSpec((1, head, head), lambda i, g, *_: (g, 0, 0)),
                pl.BlockSpec((1, head), lambda i, g, *_: (0, g)),
            ],
            out_specs=pl.BlockSpec((1, rows, head), lambda i, g, *_: (i, 0, g)),
            scratch_shapes=[
                pltpu.VMEM((8 + total, head), jnp.float32),
                pltpu.VMEM((3, 8 + total, head), jnp.float32),
            ],
        ),
        compiler_params=pltpu.CompilerParams(vmem_limit_bytes=8 * MIB),
        cost_estimate=pl.CostEstimate(
            flops=4_000_000_000, transcendentals=0, bytes_accessed=4_000_000
        ),
        name="pool_mixed",
    )(start, x, mix, scale.reshape(1, width))


def recurrent_kernel(h, p, seam_h, seam_p, entering, out):
    _, blocks, rows, _ = h.shape
    span = rows // CHUNKS
    for b in range(blocks):
        cols = slice(b * LANES, (b + 1) * LANES)
        for c in range(CHUNKS):
            one = slice(c, c + 1)
            gone_in = seam_h[0, one, cols] + seam_p[0, one, cols] * entering[0, 0:1, cols]
            at = slice(c * span, (c + 1) * span)
            out[0, at, cols] = (h[0, b, at, :] + p[0, b, at, :] * gone_in).astype(out.dtype)


def recurrent_rows(h, p, seam_h, seam_p, entering):
    seqs, blocks, rows, _ = h.shape
    width = blocks * LANES
    group = 2
    block = pl.BlockSpec((1, group, rows, LANES), lambda i, g: (i, g, 0, 0))
    seam = pl.BlockSpec((1, 2 * CHUNKS, group * LANES), lambda i, g: (i, 0, g))
    return pl.pallas_call(
        recurrent_kernel,
        out_shape=jax.ShapeDtypeStruct((seqs, rows, width), jnp.bfloat16),
        grid=(seqs, blocks // group),
        in_specs=[
            block,
            block,
            seam,
            seam,
            pl.BlockSpec((1, 1, group * LANES), lambda i, g: (i, 0, g)),
        ],
        out_specs=pl.BlockSpec((1, rows, group * LANES), lambda i, g: (i, 0, g)),
        compiler_params=pltpu.CompilerParams(vmem_limit_bytes=8 * MIB),
        cost_estimate=pl.CostEstimate(
            flops=2_000_000_000, transcendentals=0, bytes_accessed=8_000_000
        ),
    )(h, p, seam_h, seam_p, entering[:, None])


def exit_kernel(chain_spots, pool_spots, counts, shards, merged, *refs):
    if merged:
        order, side, recurrent, pooled, came, *refs = refs
    else:
        side, recurrent, pooled, *refs = refs
    chain_stacks, pool_stacks = refs[: counts[0]], refs[counts[0] : sum(counts)]
    refs = refs[sum(counts) :]
    if merged:
        out, held, sem = refs[-3:]
    else:
        (out,) = refs
    seqs, rows, _ = recurrent.shape
    half = rows // 2
    at = pl.ds(pl.multiple_of(side[0] * half, half), half)
    left = jnp.concatenate([recurrent[s, at, :] for s in range(seqs)], axis=0)
    left_pool = jnp.concatenate([pooled[s, at, :] for s in range(seqs)], axis=0)

    def columns(stacks, spots, pair):
        found = []
        for i in pair:
            stack, m = spots[shards[i]]
            found.append(stacks[stack][m])
        return jnp.concatenate(found, axis=1)

    copies = []
    for j in range(0, len(shards), 2):
        pair = range(j, min(j + 2, len(shards)))
        got = jnp.dot(
            left, columns(chain_stacks, chain_spots, pair), preferred_element_type=jnp.float32
        ) + jnp.dot(
            left_pool, columns(pool_stacks, pool_spots, pair), preferred_element_type=jnp.float32
        )
        cols = slice(j * LANES, (j + len(pair)) * LANES)
        for s in range(seqs):
            rows_of = got[s * half : (s + 1) * half]
            if merged:
                rows_of = rows_of + came[s, :, cols].astype(jnp.float32)
                held[s, :, cols] = rows_of.astype(out.dtype)
            else:
                out[s, :, cols] = rows_of.astype(out.dtype)
        if merged:
            for i in pair:
                to = pl.multiple_of(order[shards[i]] * LANES, LANES)
                copies.append(
                    pltpu.make_async_copy(
                        held.at[:, :, i * LANES : (i + 1) * LANES],
                        out.at[:, :, pl.ds(to, LANES)],
                        sem.at[i],
                    )
                )
                copies[-1].start()
    for copy in copies:
        copy.wait()


def exit_columns(side, recurrent, pooled, chain_parts, pool_parts, shards, merge=None):
    seqs, rows, width = recurrent.shape
    half = rows // 2
    wide = len(shards) * LANES

    def used(parts):
        kept = [q for q in parts if any(r in shards for r in q[1])]
        return [q[0] for q in kept], {r: (i, m) for i, q in enumerate(kept) for m, r in enumerate(q[1])}

    chain_stacks, chain_spots = used(chain_parts)
    pool_stacks, pool_spots = used(pool_parts)
    counts = (len(chain_stacks), len(pool_stacks))
    vmem = pl.BlockSpec(memory_space=pltpu.VMEM)
    smem = pl.BlockSpec(memory_space=pltpu.SMEM)
    stacks = (*chain_stacks, *pool_stacks)
    if merge is None:
        args = (side, recurrent, pooled, *stacks)
        specs = [smem] + [vmem] * (len(args) - 1)
        out_shape = jax.ShapeDtypeStruct((seqs, half, wide), jnp.bfloat16)
        extra = dict(out_specs=vmem)
    else:
        order, came, result = merge
        args = (order, side, recurrent, pooled, came, *stacks)
        specs = [smem, smem] + [vmem] * (len(args) - 2)
        aliases = {}
        if result is not None:
            args, specs = (*args, result), specs + [pl.BlockSpec(memory_space=pl.ANY)]
            aliases = {len(args) - 1: 0}
        out_shape = jax.ShapeDtypeStruct((seqs, half, order.shape[0] * LANES), jnp.bfloat16)
        extra = dict(
            out_specs=pl.BlockSpec(memory_space=pl.ANY),
            input_output_aliases=aliases,
            scratch_shapes=[
                pltpu.VMEM((seqs, half, wide), jnp.bfloat16),
                pltpu.SemaphoreType.DMA((len(shards),)),
            ],
        )
    return pl.pallas_call(
        functools.partial(exit_kernel, chain_spots, pool_spots, counts, shards, merge is not None),
        out_shape=out_shape,
        in_specs=specs,
        compiler_params=pltpu.CompilerParams(vmem_limit_bytes=18 * MIB),
        cost_estimate=pl.CostEstimate(
            flops=4 * seqs * half * width * wide, transcendentals=0, bytes_accessed=6_000_000
        ),
        **extra,
    )(*args)


def weights_and_order(chain_entry, pool_entry, chain_exit, pool_exit, width):
    sp_n, fs_n = lax.axis_size("sp"), lax.axis_size("fs")
    if chain_entry.shape[0] % LANES == 0 and chain_exit.shape[1] == LANES and fs_n == 4:
        go = lambda own, name: gather_part(own, ROUTES[name], sp_n, fs_n)
        found = go(chain_entry, "E1"), go(pool_entry, "E2"), go(chain_exit, "X1"), go(pool_exit, "X2")
        place, spot = lax.axis_index("sp"), lax.axis_index("fs")
        lap = jnp.arange(sp_n, dtype=jnp.int32)[None, :]
        swap = jnp.arange(fs_n, dtype=jnp.int32)[:, None]
        order = ((place - lap) % sp_n) * fs_n + (spot ^ swap)
        return found, order.reshape(-1).astype(jnp.int32)
    blocks = width // LANES
    places = list(range(blocks))
    entry = lambda w: [
        (lax.all_gather(w, ("sp", "fs"), axis=0, tiled=True).reshape(blocks, -1, w.shape[1]), places)
    ]
    leave = lambda w: [
        (
            lax.all_gather(w, ("sp", "fs"), axis=1, tiled=True)
            .reshape(w.shape[0], blocks, LANES)
            .transpose(1, 0, 2),
            places,
        )
    ]
    found = entry(chain_entry), entry(pool_entry), leave(chain_exit), leave(pool_exit)
    return found, jnp.arange(blocks, dtype=jnp.int32)


def per_device(
    tokens,
    norm_gain,
    chain_entry,
    pool_entry,
    conv_taps,
    recur_gate,
    input_gate,
    decay_log,
    decay_shift,
    start_state,
    pool_mix,
    pool_scale,
    chain_exit,
    pool_exit,
):
    sp_n, tp_n = lax.axis_size("sp"), lax.axis_size("tp")
    assert tp_n == 2
    _, half, width = tokens.shape
    rows = half * tp_n
    place, core = lax.axis_index("sp"), lax.axis_index("tp")
    side = jnp.reshape(core, (1,)).astype(jnp.int32)
    other_side = 1 - side
    (ce, pe, cx, px), order = weights_and_order(chain_entry, pool_entry, chain_exit, pool_exit, width)

    swap_tp = [(0, 1), (1, 0)]
    other = lax.ppermute(tokens, "tp", swap_tp)
    tail = jnp.where(core == 1, tokens[:, half - HALO :], other[:, half - HALO :])
    halo = lax.ppermute(tail, "sp", ring_pairs(sp_n))
    spot = jnp.stack([core, place]).astype(jnp.int32)
    normed = norm_rows(order, spot, tokens, other, halo, norm_gain)

    chain_input = entry_dot(normed, ce)
    pool_input = entry_dot(normed, pe)

    h, p, seam_h, seam_p = chain_scan(
        chain_input, conv_taps, recur_gate, input_gate, decay_log, decay_shift, rows * sp_n
    )
    last = jnp.stack([seam_p[:, CHUNKS], seam_h[:, CHUNKS]])
    entering = start_state
    for back in range(sp_n - 1, 0, -1):
        came = lax.ppermute(last, "sp", [(i, (i + back) % sp_n) for i in range(sp_n)])
        entering = jnp.where(place >= back, came[0] * entering + came[1], entering)

    start = jnp.reshape(place * rows, (1,)).astype(jnp.int32)
    pooled = pool_mixed(start, pool_input, pool_mix, pool_scale)

    recurrent = recurrent_rows(h, p, seam_h, seam_p, entering)

    count = order.shape[0]
    laps = sp_n if count % sp_n == 0 else count
    late = tuple(r for r in range(count) if r % laps >= laps - LATE_LAPS)
    early = tuple(r for r in range(count) if r % laps < laps - LATE_LAPS)
    ex = lambda at, shards, merge=None: exit_columns(at, recurrent, pooled, cx, px, shards, merge)
    came_early = lax.ppermute(ex(other_side, early), "tp", swap_tp)
    came_late = lax.ppermute(ex(other_side, late), "tp", swap_tp)
    result = ex(side, early, (order, came_early, None))
    return ex(side, late, (order, came_late, result))


def solution(mesh):
    in_specs = (
        P("fs", ("sp", "tp"), None),
        P(),
        P(("sp", "fs"), "tp"),
        P(("sp", "fs"), "tp"),
        P(None, "tp"),
        P("tp", None, None),
        P("tp", None, None),
        P("tp"),
        P("fs", "sp", "tp"),
        P("fs", "tp"),
        P("tp", None, None),
        P("tp"),
        P("tp", ("sp", "fs")),
        P("tp", ("sp", "fs")),
    )
    out_specs = P("fs", ("sp", "tp"), None)

    return jax.shard_map(per_device, mesh=mesh, in_specs=in_specs, out_specs=out_specs, check_vma=False)
```
